32 devices in a mesh: grp: 2 (over y), ep: 8 (over z, x), tp: 2 (over core).
Axes of the slice: x: 2, y: 2, z: 4, core: 2. Of those that a mesh axis runs over, the one named last changes fastest.
Arguments:
- tokens: bfloat16 [2048, 2048], P(('grp', 'ep')), parts along dimension 0, may hold values from -6 to 6
- in_gain: float32 [2048], replicated, may hold values from 0.1 to 1.9
- routing: int32 [2048, 4], P(('grp', 'ep')), parts along dimension 0, may hold values from 0 to 15, as said below
- gate_prob: float32 [2048, 4], P(('grp', 'ep')), parts along dimension 0, may hold values from 0.05 to 1
- w_gate: bfloat16 [16, 2048, 512], P('ep', None, 'tp'), may hold values from -0.125 to 0.125
- w_up: bfloat16 [16, 2048, 512], P('ep', None, 'tp'), may hold values from -0.125 to 0.125
- w_down: bfloat16 [16, 512, 2048], P('ep', 'tp')
- out_gain: float32 [2048], P('tp'), may hold values from 0.1 to 1.9
Outputs:
- output: bfloat16 [2048, 2048], P(('grp', 'ep'), 'tp'), parts along dimension 0
The draws below stay inside these ranges and needn't reach their ends.
There are 2 independent parts, one for each index of `grp`. The reference program is written for one: setup_inputs(seed, part) draws one part's arguments, and reference() takes and returns one part's arrays. A program takes and returns all parts, laid end to end along the dimension named above; an argument that names none is the same for every part. Nothing has to cross between parts.
Inputs may be any that keep to these rules, and one draw needn't show every extreme that they name: `routing`: each row names 4 different experts, all of one group (the same value of expert // 4). In the rows of one device no expert is named more than 64 times, and in every device's rows some expert is named exactly 64 times.
All inputs are finite; a program needn't handle non-finite values.
Results may differ from the reference program's by a relative error of at most 0.0077.
Values may be sent and summed in bfloat16 or wider, within the bound.
No kernel may reach another device: no remote copies, remote signals or barrier semaphores. Data moves between devices by JAX's collectives and lax.ppermute only.
A program may use at most 64 MiB of HBM per device.

```python
import math
import jax
import jax.numpy as jnp
from jax import lax

D = 2048
FF = 512
GROUPS = 4
TOPK = 4
TOK_DEV = 128
EXPERTS = 16
EPG = 4
TOKENS = 1024
CAP = 64
GMAX = 64
N_EP = 8
N_TP = 2


def draw_routing(key, part):
    block_count = TOKENS // TOK_DEV
    key_order, key_pick, key_perm, key_shuffle = jax.random.split(key, 4)
    hot_count = min(GMAX, TOK_DEV)
    hot_span = hot_count * TOPK // CAP
    group_order = jax.random.permutation(key_order, GROUPS)
    hot_picks = jnp.minimum(jax.random.randint(key_pick, (block_count,), 0, GROUPS + 2), GROUPS - 1)
    hot_group = group_order[hot_picks]
    position = jnp.arange(TOK_DEV, dtype=jnp.int32)
    is_hot = position < hot_count
    cold_index = position - hot_count
    groups = jnp.where(is_hot[None, :], hot_group[:, None], (hot_group[:, None] + 1 + cold_index[None, :] % (GROUPS - 1)) % GROUPS)
    group_rank = jnp.where(is_hot, position, cold_index // (GROUPS - 1))
    modulus = jnp.where(is_hot, hot_span, EPG)
    within = (group_rank[:, None] * TOPK + jnp.arange(TOPK, dtype=jnp.int32)[None, :]) % modulus[:, None]
    perm_keys = jax.random.split(key_perm, block_count * GROUPS)
    orders = jax.vmap(lambda one_key: jax.random.permutation(one_key, EPG))(perm_keys).reshape(block_count, GROUPS, EPG)
    block_ids = jnp.arange(block_count)[:, None, None]
    local_ids = orders[block_ids, groups[:, :, None], within[None, :, :]]
    experts = groups[:, :, None] * EPG + local_ids
    shuffle_keys = jax.random.split(key_shuffle, block_count)
    shuffles = jax.vmap(lambda one_key: jax.random.permutation(one_key, TOK_DEV))(shuffle_keys)
    experts = jnp.take_along_axis(experts, shuffles[:, :, None], axis=1)
    return experts.reshape(TOKENS, TOPK).astype(jnp.int32)


def draw_w_down(key, part):
    key_base, key_col = jax.random.split(key)
    columns = jnp.arange(D, dtype=jnp.float32) / D
    entries_base = jax.random.normal(key_base, (EXPERTS, FF, D), jnp.float32)
    spread = jax.random.uniform(key_col, (D,), jnp.float32, 0.5, 1.5)
    col_rise = 3.0 ** columns
    return (entries_base * FF ** (-0.5) * col_rise * spread).astype(jnp.bfloat16)


def levels(own_key, dims, cuts, low, largest):
    def one(dim, parts):
        draws = jax.random.uniform(jax.random.fold_in(jax.random.fold_in(own_key, 6), dim), (parts,), jnp.float32, low / len(cuts), largest / len(cuts))
        return jnp.repeat(jnp.exp(draws), dims[dim] // parts).reshape((-1,) + (1,) * (len(dims) - dim - 1))

    gain = one(*cuts[0])
    for cut in cuts[1:]:
        gain = gain * one(*cut)
    return gain


def bell_draw(rng, extent, width, most, cuts=(), kind=jnp.bfloat16):
    result = jax.random.normal(rng, extent, jnp.float32) * width
    if len(cuts) > 0:
        result = levels(rng, extent, cuts, -0.22, 0.18) * result
    return jnp.clip(result, min=-most, max=most).astype(kind)


def setup_inputs(seed: int = 0, part: int = 0) -> dict:
    seeds = jax.random.split(jax.random.key(seed), 9)
    part_keys = jax.random.split(jax.random.fold_in(seeds[8], part), 9)
    tokens = bell_draw(part_keys[0], (TOKENS, D), 1.0, 6.0, ((0, 8),))
    in_gain = jnp.clip(1.0 + 0.18 * jax.random.normal(seeds[1], (D,), jnp.float32), 0.1, 1.9)
    routing = draw_routing(jax.random.fold_in(jax.random.fold_in(seeds[8], part), 71), part)
    gate_prob = jnp.clip(jnp.exp(math.log(1.0) - 2.9957323 * jax.random.uniform(part_keys[3], (TOKENS, TOPK), jnp.float32) ** levels(part_keys[3], (TOKENS, TOPK), ((0, 8),), -0.2, 0.2)), 0.05, 1.0)
    w_gate = bell_draw(seeds[4], (EXPERTS, D, FF), D ** -0.5, 0.125, ((0, 8), (2, 2)))
    w_up = bell_draw(seeds[5], (EXPERTS, D, FF), D ** -0.5, 0.125, ((0, 8), (2, 2)))
    w_down = draw_w_down(jax.random.fold_in(seeds[8], 71), part)
    out_gain = jnp.clip(1.0 + 0.18 * jax.random.normal(seeds[7], (D,), jnp.float32), 0.1, 1.9)
    return dict(tokens=tokens, in_gain=in_gain, routing=routing, gate_prob=gate_prob, w_gate=w_gate, w_up=w_up, w_down=w_down, out_gain=out_gain)


EPS = 1e-06

def slot_ranks(flat_routes):
    matches = (flat_routes[:, None] == jnp.arange(EXPERTS, dtype=jnp.int32)[None, :]).astype(jnp.int32)
    earlier = jnp.cumsum(matches, axis=0) - matches
    return lax.optimization_barrier(jnp.sum(earlier * matches, axis=1)).astype(jnp.int32)

def reference(tokens, in_gain, routing, gate_prob, w_gate, w_up, w_down, out_gain):
    floats = tokens.astype(jnp.float32)
    normed = (floats * lax.rsqrt(lax.optimization_barrier(jnp.mean(floats * floats, axis=-1, keepdims=True)) + EPS) * in_gain).astype(jnp.bfloat16)
    blocks = routing.reshape(N_EP, TOK_DEV * TOPK)
    slot_rank = jax.vmap(slot_ranks)(blocks)
    sources = jnp.arange(N_EP, dtype=jnp.int32)[:, None]
    slot_ids = (blocks * (N_EP * CAP) + sources * CAP + slot_rank).reshape(-1).astype(jnp.int32)
    token_ids = jnp.arange(TOKENS * TOPK, dtype=jnp.int32) // TOPK
    slot_table = jnp.zeros((EXPERTS * N_EP * CAP,), jnp.int32).at[slot_ids].set(token_ids + 1)
    slot_table = slot_table.reshape(EXPERTS, N_EP * CAP)

    def expert(inputs):
        entries, gate_w, up_w, down_w = inputs
        filled = entries > 0
        rows_in = jnp.where(filled[:, None], normed[jnp.maximum(entries - 1, 0)], jnp.zeros((), jnp.bfloat16))
        gate_act = jnp.dot(rows_in, gate_w, preferred_element_type=jnp.float32)
        up_act = jnp.dot(rows_in, up_w, preferred_element_type=jnp.float32)
        hidden = (jax.nn.silu(gate_act) * up_act).astype(jnp.bfloat16)
        pieces = jnp.einsum('rnf,nfd->nrd', hidden.reshape(-1, N_TP, FF // N_TP).astype(jnp.float32), down_w.reshape(N_TP, FF // N_TP, D).astype(jnp.float32))
        rounded = lax.optimization_barrier(pieces.astype(jnp.bfloat16))
        return lax.optimization_barrier(jnp.sum(rounded.astype(jnp.float32), axis=0)).astype(jnp.bfloat16)
    results = lax.map(expert, (slot_table, w_gate, w_up, w_down))
    picked = results.reshape(-1, D)[slot_ids].astype(jnp.float32).reshape(TOKENS, TOPK, D)
    mixed_rows = lax.optimization_barrier(jnp.sum(picked * gate_prob[:, :, None], axis=1))
    inv_rms = lax.rsqrt(lax.optimization_barrier(jnp.mean(mixed_rows * mixed_rows, axis=-1, keepdims=True)) + EPS)
    return (mixed_rows * inv_rms * out_gain).astype(jnp.bfloat16)
```

```python
import functools

import jax
import jax.numpy as jnp
from jax import lax
from jax.experimental import pallas as pl
from jax.experimental.pallas import tpu as pltpu
from jax.sharding import PartitionSpec as P

GROUPS = 4


EPS = 1e-06
LANES = 128
TERMS = 3
MIB = 1 << 20


def slot_ranks(flat_routes, expert_count):
    matches = (flat_routes[:, None] == jnp.arange(expert_count, dtype=jnp.int32)[None, :]).astype(
        jnp.int32
    )
    earlier = jnp.cumsum(matches, axis=0) - matches
    return jnp.sum(earlier * matches, axis=1)


def fill_rows(source, entries):
    filled = entries > 0
    return jnp.where(
        filled[:, None], source[jnp.maximum(entries - 1, 0)], jnp.zeros((), source.dtype)
    )


def sparse_body(tokens, in_gain, routing, gate_prob, w_gate, w_up, w_down, out_gain):
    ep_count = lax.axis_size("ep")
    local_experts = w_gate.shape[0]
    expert_count = local_experts * ep_count
    tok_dev, top_count = routing.shape
    model_width = tokens.shape[1]
    half_width = out_gain.shape[0]
    group_width = expert_count // GROUPS
    row_cap = max(2, tok_dev * top_count // (2 * group_width))
    floats = tokens.astype(jnp.float32)
    normed = (
        floats * lax.rsqrt(jnp.mean(floats * floats, axis=-1, keepdims=True) + EPS) * in_gain
    ).astype(jnp.bfloat16)
    flat_routes = routing.reshape(-1)
    slot_rank = slot_ranks(flat_routes, expert_count)
    slot_ids = flat_routes * row_cap + slot_rank
    token_ids = jnp.arange(tok_dev * top_count, dtype=jnp.int32) // top_count
    slot_table = jnp.zeros((expert_count * row_cap,), jnp.int32).at[slot_ids].set(token_ids + 1)
    own_columns = lax.dynamic_slice_in_dim(normed, lax.axis_index("tp") * half_width, half_width, 1)
    sendbuf = fill_rows(own_columns, slot_table).reshape(
        ep_count, local_experts, row_cap, half_width
    )
    arrived = lax.all_to_all(sendbuf, "ep", split_axis=0, concat_axis=0, tiled=True)
    arrived = lax.all_gather(arrived, "tp", axis=3, tiled=True)
    gate_act = jnp.einsum("secd,edf->secf", arrived, w_gate, preferred_element_type=jnp.float32)
    up_act = jnp.einsum("secd,edf->secf", arrived, w_up, preferred_element_type=jnp.float32)
    hidden = (jax.nn.silu(gate_act) * up_act).astype(jnp.bfloat16)
    partial_out = jnp.einsum("secf,efd->secd", hidden, w_down, preferred_element_type=jnp.float32)
    results = lax.psum_scatter(
        partial_out.astype(jnp.bfloat16), "tp", scatter_dimension=3, tiled=True
    )
    returned = lax.all_to_all(results, "ep", split_axis=0, concat_axis=0, tiled=True).reshape(
        expert_count * row_cap, half_width
    )
    picked = returned[slot_ids].astype(jnp.float32).reshape(tok_dev, top_count, half_width)
    mixed_rows = jnp.sum(picked * gate_prob[:, :, None], axis=1)
    squares = jnp.sum(mixed_rows * mixed_rows, axis=1)
    total_squares = lax.psum(squares, "tp")
    inv_rms = lax.rsqrt(total_squares / model_width + EPS)
    return (mixed_rows * inv_rms[:, None] * out_gain).astype(jnp.bfloat16)


def dot(a, b):
    return jnp.dot(a, b, preferred_element_type=jnp.float32)


def pack_kernel(members, width, cap, tok_ref, gain_ref, route_ref, prob_ref, *outs):
    half = cap // 2
    my_group = lax.axis_index("ep") // members
    my_half = lax.axis_index("tp")
    floats = tok_ref[...].astype(jnp.float32)
    tok_dev, model_width = floats.shape
    inv = lax.rsqrt(jnp.sum(floats * floats, axis=-1, keepdims=True) / model_width + EPS)
    normed = (floats * inv * gain_ref[...]).astype(jnp.bfloat16)
    routes = route_ref[...]
    probs = prob_ref[...]
    first = routes[:, 0:1]
    group = jnp.zeros_like(first)
    for g in range(1, GROUPS):
        group += (first >= g * width).astype(jnp.int32)
    lane = lax.broadcasted_iota(jnp.int32, (tok_dev, LANES), 1)
    member = (group == lane).astype(jnp.float32)
    row = lax.broadcasted_iota(jnp.int32, (tok_dev, tok_dev), 0)
    col = lax.broadcasted_iota(jnp.int32, (tok_dev, tok_dev), 1)
    earlier = dot((col < row).astype(jnp.bfloat16), member.astype(jnp.bfloat16))
    rank = jnp.sum(earlier * member, axis=1, keepdims=True).astype(jnp.int32)
    relative = group ^ my_group
    send_slot = lax.broadcasted_iota(jnp.int32, (tok_dev, GROUPS * half), 1)
    pick = (
        (relative == send_slot // half) & (rank == send_slot % half + my_half * half)
    ).astype(jnp.bfloat16)
    lane_expert = lane % width
    weight = jnp.zeros((tok_dev, LANES), jnp.float32)
    for k in range(routes.shape[1]):
        weight += jnp.where(routes[:, k : k + 1] - group * width == lane_expert, probs[:, k : k + 1], 0.0)
    high = weight.astype(jnp.bfloat16)
    rest = weight - high.astype(jnp.float32)
    middle = rest.astype(jnp.bfloat16)
    low = (rest - middle.astype(jnp.float32)).astype(jnp.bfloat16)
    zero = jnp.zeros_like(high)
    terms = jnp.where(
        lane < width,
        high,
        jnp.where(lane < 2 * width, middle, jnp.where(lane < TERMS * width, low, zero)),
    )
    contract = (((0,), (0,)), ((), ()))
    rows = lax.dot_general(pick, normed, contract, preferred_element_type=jnp.float32)
    extra = lax.dot_general(pick, terms, contract, preferred_element_type=jnp.float32)
    for k in range(GROUPS):
        outs[k][:, :model_width] = rows[k * half : (k + 1) * half].astype(jnp.bfloat16)
        outs[k][:, model_width:] = extra[k * half : (k + 1) * half].astype(jnp.bfloat16)
    slot = lax.broadcasted_iota(jnp.int32, (tok_dev, GROUPS * cap), 1)
    outs[GROUPS][...] = (relative * cap + rank == slot).astype(jnp.bfloat16)


def expert_kernel(chunks, members, width, half, *refs):
    pieces = refs[: 4 * chunks]
    wg_ref, wu_ref, wd_ref, keep_ref, send_ref, rows_ref = refs[4 * chunks :]
    my_half = lax.axis_index("tp")
    me = lax.axis_index("ep") % members
    local_experts, model_width, hidden_width = wg_ref.shape
    half_width = keep_ref.shape[1]
    mine = pl.multiple_of(my_half * half, half)
    other = pl.multiple_of((1 - my_half) * half, half)
    for c in range(chunks):
        own, own_tp, far, far_tp = pieces[4 * c : 4 * c + 4]
        near_base = c * 4 * half
        far_base = near_base + 2 * half
        rows_ref[pl.ds(near_base + mine, half), :] = own[...]
        rows_ref[pl.ds(near_base + other, half), :] = own_tp[...]
        rows_ref[pl.ds(far_base + mine, half), :] = far[...]
        rows_ref[pl.ds(far_base + other, half), :] = far_tp[...]
    rows = rows_ref[:, :model_width]
    terms = rows_ref[:, model_width:].astype(jnp.float32)
    lane = lax.broadcasted_iota(jnp.int32, terms.shape, 1)
    hidden = []
    for e in range(local_experts):
        wanted = (lane % width == me * local_experts + e) & (lane < TERMS * width)
        weight = jnp.sum(jnp.where(wanted, terms, 0.0), axis=1, keepdims=True)
        gate_act = dot(rows, wg_ref[e])
        up_act = dot(rows, wu_ref[e])
        act = gate_act / (1.0 + jnp.exp(-gate_act)) * up_act
        hidden.append((act * weight).astype(jnp.bfloat16))
    send_at = pl.multiple_of((1 - my_half) * half_width, half_width)
    keep_at = pl.multiple_of(my_half * half_width, half_width)
    total = dot(hidden[0], wd_ref[0, :, pl.ds(send_at, half_width)])
    for e in range(1, local_experts):
        total += dot(hidden[e], wd_ref[e, :, pl.ds(send_at, half_width)])
    send_ref[...] = total.astype(jnp.bfloat16)
    total = dot(hidden[0], wd_ref[0, :, pl.ds(keep_at, half_width)])
    for e in range(1, local_experts):
        total += dot(hidden[e], wd_ref[e, :, pl.ds(keep_at, half_width)])
    keep_ref[...] = total


def split_kernel(chunks, cap, mine_ref, recv_ref, keep_ref, send_ref):
    for c in range(chunks):
        near = pl.ds(2 * c * cap, cap)
        far = pl.ds((2 * c + 1) * cap, cap)
        out = pl.ds(c * cap, cap)
        keep_ref[out, :] = mine_ref[near, :] + recv_ref[near, :].astype(jnp.float32)
        send_ref[out, :] = (mine_ref[far, :] + recv_ref[far, :].astype(jnp.float32)).astype(
            jnp.bfloat16
        )


def join_kernel(chunks, cap, keep_ref, recv_ref, *outs):
    for c in range(chunks):
        at = pl.ds(c * cap, cap)
        outs[c][...] = (keep_ref[at, :] + recv_ref[at, :].astype(jnp.float32)).astype(jnp.bfloat16)


def place_kernel(cap, map_ref, *refs):
    parts = refs[:GROUPS]
    mixed_ref, square_ref = refs[GROUPS:]
    mixed = dot(map_ref[:, :cap], parts[0][...])
    for k in range(1, GROUPS):
        mixed += dot(map_ref[:, k * cap : (k + 1) * cap], parts[k][...])
    mixed_ref[...] = mixed
    square_ref[...] = jnp.broadcast_to(
        jnp.sum(mixed * mixed, axis=1, keepdims=True), square_ref.shape
    )


def close_kernel(model_width, mixed_ref, mine_ref, other_ref, gain_ref, out_ref):
    squares = (mine_ref[...] + other_ref[...])[:, 0:1]
    inv = lax.rsqrt(squares / model_width + EPS)
    out_ref[...] = (mixed_ref[...] * inv * gain_ref[...]).astype(jnp.bfloat16)


def call(kernel, outs, args, name, limit, flops, scratch=()):
    return pl.pallas_call(
        kernel,
        out_shape=outs,
        scratch_shapes=scratch,
        name=name,
        compiler_params=pltpu.CompilerParams(vmem_limit_bytes=limit * MIB),
        cost_estimate=pl.CostEstimate(flops=flops, transcendentals=0, bytes_accessed=0),
    )(*args)


def dense_body(tokens, in_gain, routing, gate_prob, w_gate, w_up, w_down, out_gain):
    ep_count = lax.axis_size("ep")
    local_experts, model_width, hidden_width = w_gate.shape
    tok_dev, top_count = routing.shape
    half_width = out_gain.shape[0]
    width = local_experts * ep_count // GROUPS
    members = width // local_experts
    cap = tok_dev * top_count // (2 * width)
    half = cap // 2
    sds = jax.ShapeDtypeStruct
    bf16, f32 = jnp.bfloat16, jnp.float32
    block = sds((half, model_width + LANES), bf16)

    def hop(value, k):
        pairs = [(i, ((i // members) ^ k) * members + i % members) for i in range(ep_count)]
        return lax.ppermute(value, "ep", pairs)

    def cross(value):
        pairs = [(i, i ^ 1) for i in range(ep_count)]
        return lax.ppermute(value, "ep", pairs)

    def swap(value):
        return lax.ppermute(value, "tp", [(0, 1), (1, 0)])

    packed = call(
        functools.partial(pack_kernel, members, width, cap),
        [block] * GROUPS + [sds((tok_dev, GROUPS * cap), bf16)],
        (tokens, in_gain.reshape(1, -1), routing, gate_prob),
        "pack",
        12,
        2 * tok_dev * tok_dev * model_width,
    )
    token_map = packed[GROUPS]
    arrived = [packed[0]] + [hop(packed[k], k) for k in range(1, GROUPS)]

    def experts(ks):
        pieces = []
        for k in ks:
            far = cross(arrived[k])
            pieces += [arrived[k], swap(arrived[k]), far, swap(far)]
        n = len(ks)
        rows = n * 2 * cap
        mine, other = call(
            functools.partial(expert_kernel, n, members, width, half),
            [sds((rows, half_width), f32), sds((rows, half_width), bf16)],
            (*pieces, w_gate, w_up, w_down),
            "experts",
            24,
            6 * rows * model_width * hidden_width * local_experts,
            (pltpu.VMEM((rows, model_width + LANES), bf16),),
        )
        keep, send = call(
            functools.partial(split_kernel, n, cap),
            [sds((n * cap, half_width), f32), sds((n * cap, half_width), bf16)],
            (mine, swap(other)),
            "split",
            8,
            rows * half_width,
        )
        return call(
            functools.partial(join_kernel, n, cap),
            [sds((cap, half_width), bf16)] * n,
            (keep, cross(send)),
            "join",
            8,
            rows * half_width,
        )

    step = GROUPS // 2
    first = experts(range(step))
    second = experts(range(step, GROUPS))
    done = list(first) + list(second)
    back = [done[0]] + [hop(done[k], k) for k in range(1, GROUPS)]
    mixed, squares = call(
        functools.partial(place_kernel, cap),
        [sds((tok_dev, half_width), f32), sds((tok_dev, LANES), f32)],
        (token_map, *back),
        "place",
        8,
        2 * tok_dev * GROUPS * cap * half_width,
    )
    return call(
        functools.partial(close_kernel, model_width),
        sds((tok_dev, half_width), bf16),
        (mixed, squares, swap(squares), out_gain.reshape(1, -1)),
        "close",
        8,
        tok_dev * half_width,
    )


def solution(mesh):
    placed = (
        P(("grp", "ep"), None),
        P(),
        P(("grp", "ep"), None),
        P(("grp", "ep"), None),
        P("ep", None, "tp"),
        P("ep", None, "tp"),
        P("ep", "tp", None),
        P("tp"),
    )

    def body(*args):
        routing, w_gate = args[2], args[4]
        width = w_gate.shape[0] * mesh.shape["ep"] // GROUPS
        dense = routing.shape[1] == width and width == 2 * w_gate.shape[0] and mesh.shape["tp"] == 2
        return (dense_body if dense else sparse_body)(*args)

    return jax.shard_map(
        body, mesh=mesh, in_specs=placed, out_specs=P(("grp", "ep"), "tp"), check_vma=False
    )
```

```python
import functools

import jax
import jax.numpy as jnp
from jax import lax
from jax.experimental import pallas as pl
from jax.experimental.pallas import tpu as pltpu
from jax.sharding import PartitionSpec as P

GROUPS = 4


EPS = 1e-06
LANES = 128
TERMS = 3
MIB = 1 << 20


def slot_ranks(flat_routes, expert_count):
    matches = (flat_routes[:, None] == jnp.arange(expert_count, dtype=jnp.int32)[None, :]).astype(
        jnp.int32
    )
    earlier = jnp.cumsum(matches, axis=0) - matches
    return jnp.sum(earlier * matches, axis=1)


def fill_rows(source, entries):
    filled = entries > 0
    return jnp.where(
        filled[:, None], source[jnp.maximum(entries - 1, 0)], jnp.zeros((), source.dtype)
    )


def sparse_body(tokens, in_gain, routing, gate_prob, w_gate, w_up, w_down, out_gain):
    ep_count = lax.axis_size("ep")
    local_experts = w_gate.shape[0]
    expert_count = local_experts * ep_count
    tok_dev, top_count = routing.shape
    model_width = tokens.shape[1]
    half_width = out_gain.shape[0]
    group_width = expert_count // GROUPS
    row_cap = max(2, tok_dev * top_count // (2 * group_width))
    floats = tokens.astype(jnp.float32)
    normed = (
        floats * lax.rsqrt(jnp.mean(floats * floats, axis=-1, keepdims=True) + EPS) * in_gain
    ).astype(jnp.bfloat16)
    flat_routes = routing.reshape(-1)
    slot_rank = slot_ranks(flat_routes, expert_count)
    slot_ids = flat_routes * row_cap + slot_rank
    token_ids = jnp.arange(tok_dev * top_count, dtype=jnp.int32) // top_count
    slot_table = jnp.zeros((expert_count * row_cap,), jnp.int32).at[slot_ids].set(token_ids + 1)
    own_columns = lax.dynamic_slice_in_dim(normed, lax.axis_index("tp") * half_width, half_width, 1)
    sendbuf = fill_rows(own_columns, slot_table).reshape(
        ep_count, local_experts, row_cap, half_width
    )
    arrived = lax.all_to_all(sendbuf, "ep", split_axis=0, concat_axis=0, tiled=True)
    arrived = lax.all_gather(arrived, "tp", axis=3, tiled=True)
    gate_act = jnp.einsum("secd,edf->secf", arrived, w_gate, preferred_element_type=jnp.float32)
    up_act = jnp.einsum("secd,edf->secf", arrived, w_up, preferred_element_type=jnp.float32)
    hidden = (jax.nn.silu(gate_act) * up_act).astype(jnp.bfloat16)
    partial_out = jnp.einsum("secf,efd->secd", hidden, w_down, preferred_element_type=jnp.float32)
    results = lax.psum_scatter(
        partial_out.astype(jnp.bfloat16), "tp", scatter_dimension=3, tiled=True
    )
    returned = lax.all_to_all(results, "ep", split_axis=0, concat_axis=0, tiled=True).reshape(
        expert_count * row_cap, half_width
    )
    picked = returned[slot_ids].astype(jnp.float32).reshape(tok_dev, top_count, half_width)
    mixed_rows = jnp.sum(picked * gate_prob[:, :, None], axis=1)
    squares = jnp.sum(mixed_rows * mixed_rows, axis=1)
    total_squares = lax.psum(squares, "tp")
    inv_rms = lax.rsqrt(total_squares / model_width + EPS)
    return (mixed_rows * inv_rms[:, None] * out_gain).astype(jnp.bfloat16)


def dot(a, b):
    return jnp.dot(a, b, preferred_element_type=jnp.float32)


def iota(shape, dim):
    return lax.broadcasted_iota(jnp.int32, shape, dim)


def pack_kernel(members, width, cap, *refs):
    sources, refs = refs[:4], refs[4:]
    outs, map_ref, refs = refs[:GROUPS], refs[GROUPS], refs[GROUPS + 1 :]
    copies = [
        pltpu.make_async_copy(source, target, refs[4].at[i])
        for i, (source, target) in enumerate(zip(sources, refs[:4]))
    ]
    for copy in copies:
        copy.start()
    tok_ref, gain_ref, route_ref, prob_ref = refs[:4]
    half = cap // 2
    my_group = lax.axis_index("ep") // members
    my_half = lax.axis_index("tp")
    tok_dev, model_width = tok_ref.shape
    copies[2].wait()
    copies[3].wait()
    routes = route_ref[...]
    probs = prob_ref[...]
    first = routes[0:1]
    group = jnp.zeros_like(first)
    for g in range(1, GROUPS):
        group += (first >= g * width).astype(jnp.int32)
    member = (group == iota((8, tok_dev), 0)).astype(jnp.float32)
    before = (iota((tok_dev, tok_dev), 0) < iota((tok_dev, tok_dev), 1)).astype(jnp.bfloat16)
    earlier = dot(member.astype(jnp.bfloat16), before)
    rank = jnp.sum(earlier * member, axis=0, keepdims=True).astype(jnp.int32)
    relative = group ^ my_group
    send_slot = iota((GROUPS * half, tok_dev), 0)
    pick = (
        (relative == send_slot // half) & (rank == send_slot % half + my_half * half)
    ).astype(jnp.bfloat16)
    lane = iota((LANES, tok_dev), 0)
    weight = jnp.zeros((LANES, tok_dev), jnp.float32)
    for k in range(routes.shape[0]):
        weight += jnp.where(
            routes[k : k + 1] - group * width == lane % width, probs[k : k + 1], 0.0
        )
    high = weight.astype(jnp.bfloat16).astype(jnp.float32)
    rest = weight - high
    middle = rest.astype(jnp.bfloat16).astype(jnp.float32)
    low = rest - middle
    terms = jnp.where(
        lane < width,
        high,
        jnp.where(lane < 2 * width, middle, jnp.where(lane < TERMS * width, low, 0.0)),
    ).astype(jnp.bfloat16)
    extra = lax.dot_general(
        pick, terms, (((1,), (1,)), ((), ())), preferred_element_type=jnp.float32
    ).astype(jnp.bfloat16)
    map_ref[...] = (relative * cap + rank == iota((GROUPS * cap, tok_dev), 0)).astype(jnp.bfloat16)
    copies[0].wait()
    copies[1].wait()
    floats = tok_ref[...].astype(jnp.float32)
    inv = lax.rsqrt(jnp.sum(floats * floats, axis=-1, keepdims=True) / model_width + EPS)
    normed = (floats * inv * gain_ref[...]).astype(jnp.bfloat16)
    rows = dot(pick, normed).astype(jnp.bfloat16)
    for k in range(GROUPS):
        outs[k][:, :model_width] = rows[k * half : (k + 1) * half]
        outs[k][:, model_width:] = extra[k * half : (k + 1) * half]


def load_kernel(wg_ref, wu_ref, wd_ref, map_ref, wg_out, wu_out, wd_out, map_out, sems):
    copies = [
        pltpu.make_async_copy(source.at[e], target.at[e], sems.at[i, e])
        for i, (source, target) in enumerate(
            ((wg_ref, wg_out), (wu_ref, wu_out), (wd_ref, wd_out))
        )
        for e in range(wg_ref.shape[0])
    ]
    for copy in copies:
        copy.start()
    map_out[...] = map_ref[...].astype(jnp.float32).T.astype(jnp.bfloat16)
    for copy in copies:
        copy.wait()


def expert_kernel(chunks, members, width, half, *refs):
    pieces = refs[: 4 * chunks]
    wg_ref, wu_ref, wd_ref, keep_ref, send_ref, rows_ref = refs[4 * chunks :]
    my_half = lax.axis_index("tp")
    me = lax.axis_index("ep") % members
    local_experts, model_width, _ = wg_ref.shape
    half_width = keep_ref.shape[1]
    mine = pl.multiple_of(my_half * half, half)
    other = pl.multiple_of((1 - my_half) * half, half)
    for c in range(chunks):
        own, own_tp, far, far_tp = pieces[4 * c : 4 * c + 4]
        near_base = c * 4 * half
        far_base = near_base + 2 * half
        rows_ref[pl.ds(near_base + mine, half), :] = own[...]
        rows_ref[pl.ds(near_base + other, half), :] = own_tp[...]
        rows_ref[pl.ds(far_base + mine, half), :] = far[...]
        rows_ref[pl.ds(far_base + other, half), :] = far_tp[...]
    rows = rows_ref[:, :model_width]
    terms = rows_ref[:, model_width:].astype(jnp.float32)
    lane = lax.broadcasted_iota(jnp.int32, terms.shape, 1)
    hidden = []
    for e in range(local_experts):
        wanted = (lane % width == me * local_experts + e) & (lane < TERMS * width)
        weight = jnp.sum(jnp.where(wanted, terms, 0.0), axis=1, keepdims=True)
        gate_act = dot(rows, wg_ref[e])
        up_act = dot(rows, wu_ref[e])
        act = gate_act / (1.0 + jnp.exp(-gate_act)) * up_act
        hidden.append((act * weight).astype(jnp.bfloat16))
    send_at = pl.multiple_of((1 - my_half) * half_width, half_width)
    keep_at = pl.multiple_of(my_half * half_width, half_width)
    total = dot(hidden[0], wd_ref[0, :, pl.ds(send_at, half_width)])
    for e in range(1, local_experts):
        total += dot(hidden[e], wd_ref[e, :, pl.ds(send_at, half_width)])
    send_ref[...] = total.astype(jnp.bfloat16)
    total = dot(hidden[0], wd_ref[0, :, pl.ds(keep_at, half_width)])
    for e in range(1, local_experts):
        total += dot(hidden[e], wd_ref[e, :, pl.ds(keep_at, half_width)])
    keep_ref[...] = total


def split_kernel(chunks, cap, mine_ref, recv_ref, *outs):
    for c in range(chunks):
        near = pl.ds(2 * c * cap, cap)
        far = pl.ds((2 * c + 1) * cap, cap)
        keep_ref, send_ref = outs[2 * c : 2 * c + 2]
        keep_ref[...] = mine_ref[near, :] + recv_ref[near, :].astype(jnp.float32)
        send_ref[...] = (mine_ref[far, :] + recv_ref[far, :].astype(jnp.float32)).astype(
            jnp.bfloat16
        )


def join_kernel(keep_ref, recv_ref, row_ref, square_ref):
    rows = keep_ref[...] + recv_ref[...].astype(jnp.float32)
    row_ref[...] = rows.astype(jnp.bfloat16)
    squares = jnp.sum(rows * rows, axis=1, keepdims=True)
    square_ref[...] = jnp.broadcast_to(squares, (rows.shape[0], LANES)).T[:8]


def close_kernel(cap, model_width, map_ref, gain_ref, *refs):
    parts, squares = refs[:GROUPS], refs[GROUPS : 2 * GROUPS]
    out_ref, rows_ref = refs[2 * GROUPS :]
    for k in range(GROUPS):
        rows_ref[k * cap : (k + 1) * cap, :] = parts[k][...]
    placing = map_ref[...]
    mixed = dot(placing, rows_ref[...])
    far = jnp.concatenate([square[0:1, :] for square in squares], axis=1)
    total = jnp.sum(mixed * mixed, axis=1, keepdims=True) + jnp.sum(
        placing.astype(jnp.float32) * far, axis=1, keepdims=True
    )
    out_ref[...] = (mixed * lax.rsqrt(total / model_width + EPS) * gain_ref[...]).astype(
        jnp.bfloat16
    )


def call(kernel, outs, args, limit, scratch=(), in_specs=None):
    return pl.pallas_call(
        kernel,
        out_shape=outs,
        in_specs=in_specs or [pl.BlockSpec(memory_space=pltpu.VMEM)] * len(args),
        scratch_shapes=scratch,
        compiler_params=pltpu.CompilerParams(vmem_limit_bytes=limit * MIB),
    )(*args)


def dense_body(tokens, in_gain, routing, gate_prob, w_gate, w_up, w_down, out_gain):
    ep_count = lax.axis_size("ep")
    local_experts, model_width, _ = w_gate.shape
    tok_dev, top_count = routing.shape
    half_width = out_gain.shape[0]
    width = local_experts * ep_count // GROUPS
    members = width // local_experts
    cap = tok_dev * top_count // (2 * width)
    half = cap // 2
    sds = jax.ShapeDtypeStruct
    bf16, f32 = jnp.bfloat16, jnp.float32
    block = sds((half, model_width + LANES), bf16)
    anywhere = pl.BlockSpec(memory_space=pltpu.HBM)
    in_vmem = pl.BlockSpec(memory_space=pltpu.VMEM)

    def far_ep(i, k):
        return ((i // members) ^ k) * members + i % members

    def hop(value, k):
        return lax.ppermute(value, "ep", [(i, far_ep(i, k)) for i in range(ep_count)])

    def hop_swap(value, k):
        pairs = [
            (2 * i + t, 2 * far_ep(i, k) + 1 - t) for i in range(ep_count) for t in range(2)
        ]
        return lax.ppermute(value, ("ep", "tp"), pairs)

    def cross(value):
        return lax.ppermute(value, "ep", [(i, i ^ 1) for i in range(ep_count)])

    def swap(value):
        return lax.ppermute(value, "tp", [(0, 1), (1, 0)])

    def held(value):
        return pltpu.with_memory_space_constraint(value, pltpu.HBM)

    routes_t, probs_t = held(routing.T), held(gate_prob.T)
    tokens, gain_row = held(tokens), held(in_gain.reshape(1, -1))
    w_gate, w_up, w_down = held(w_gate), held(w_up), held(w_down)
    *packed, slot_map = call(
        functools.partial(pack_kernel, members, width, cap),
        [block] * GROUPS + [sds((GROUPS * cap, tok_dev), bf16)],
        (tokens, gain_row, routes_t, probs_t),
        12,
        (
            pltpu.VMEM(tokens.shape, bf16),
            pltpu.VMEM((1, model_width), f32),
            pltpu.VMEM(routes_t.shape, jnp.int32),
            pltpu.VMEM(probs_t.shape, f32),
            pltpu.SemaphoreType.DMA((4,)),
        ),
        [anywhere] * 4,
    )
    *weights, token_map = call(
        load_kernel,
        [sds(w.shape, bf16) for w in (w_gate, w_up, w_down)]
        + [sds((tok_dev, GROUPS * cap), bf16)],
        (w_gate, w_up, w_down, slot_map),
        12,
        (pltpu.SemaphoreType.DMA((3, local_experts)),),
        [anywhere] * 3 + [in_vmem],
    )
    arrived = [packed[0]] + [hop(packed[k], k) for k in range(1, GROUPS)]

    back, squares = [None] * GROUPS, [None] * GROUPS

    def experts(ks):
        pieces = []
        for k in ks:
            far = cross(arrived[k])
            pieces += [arrived[k], swap(arrived[k]), far, swap(far)]
        n = len(ks)
        rows = n * 2 * cap
        mine, other = call(
            functools.partial(expert_kernel, n, members, width, half),
            [sds((rows, half_width), f32), sds((rows, half_width), bf16)],
            (*pieces, *weights),
            24,
            (pltpu.VMEM((rows, model_width + LANES), bf16),),
        )
        split = call(
            functools.partial(split_kernel, n, cap),
            [sds((cap, half_width), f32), sds((cap, half_width), bf16)] * n,
            (mine, swap(other)),
            8,
        )
        for c, k in enumerate(ks):
            keep, send = split[2 * c : 2 * c + 2]
            rows_out, square = call(
                join_kernel,
                [sds((cap, half_width), bf16), sds((8, cap), f32)],
                (keep, cross(send)),
                8,
            )
            if k == 0:
                back[k], squares[k] = rows_out, swap(square)
            else:
                back[k] = hop(rows_out, k)
                squares[k] = hop_swap(square, k)

    for ks in STAGES:
        experts(ks)
    return call(
        functools.partial(close_kernel, cap, model_width),
        sds((tok_dev, half_width), bf16),
        (token_map, out_gain.reshape(1, -1), *back, *squares),
        8,
        (pltpu.VMEM((GROUPS * cap, half_width), bf16),),
    )


STAGES = ((0, 1), (3,), (2,))


def solution(mesh):
    placed = (
        P(("grp", "ep"), None),
        P(),
        P(("grp", "ep"), None),
        P(("grp", "ep"), None),
        P("ep", None, "tp"),
        P("ep", None, "tp"),
        P("ep", "tp", None),
        P("tp"),
    )

    def step(*args):
        routing, w_gate = args[2], args[4]
        width = w_gate.shape[0] // GROUPS
        members = mesh.shape["ep"] // GROUPS
        dense = routing.shape[1] == width and members == 2 and mesh.shape["tp"] == 2

        def body(*shards):
            return (dense_body if dense else sparse_body)(*shards)

        whole = jax.shard_map(
            body, mesh=mesh, in_specs=placed, out_specs=P(("grp", "ep"), "tp"), check_vma=False
        )
        return whole(*args)

    return step
```

```python
import functools

import jax
import jax.numpy as jnp
from jax import lax
from jax.experimental import pallas as pl
from jax.experimental.pallas import tpu as pltpu
from jax.sharding import PartitionSpec as P

GROUPS = 4


EPS = 1e-06
LANES = 128
TERMS = 3
MIB = 1 << 20


def slot_ranks(flat_routes, expert_count):
    matches = (flat_routes[:, None] == jnp.arange(expert_count, dtype=jnp.int32)[None, :]).astype(
        jnp.int32
    )
    earlier = jnp.cumsum(matches, axis=0) - matches
    return jnp.sum(earlier * matches, axis=1)


def fill_rows(source, entries):
    filled = entries > 0
    return jnp.where(
        filled[:, None], source[jnp.maximum(entries - 1, 0)], jnp.zeros((), source.dtype)
    )


def sparse_body(tokens, in_gain, routing, gate_prob, w_gate, w_up, w_down, out_gain):
    ep_count = lax.axis_size("ep")
    local_experts = w_gate.shape[0]
    expert_count = local_experts * ep_count
    tok_dev, top_count = routing.shape
    model_width = tokens.shape[1]
    half_width = out_gain.shape[0]
    group_width = expert_count // GROUPS
    row_cap = max(2, tok_dev * top_count // (2 * group_width))
    floats = tokens.astype(jnp.float32)
    normed = (
        floats * lax.rsqrt(jnp.mean(floats * floats, axis=-1, keepdims=True) + EPS) * in_gain
    ).astype(jnp.bfloat16)
    flat_routes = routing.reshape(-1)
    slot_rank = slot_ranks(flat_routes, expert_count)
    slot_ids = flat_routes * row_cap + slot_rank
    token_ids = jnp.arange(tok_dev * top_count, dtype=jnp.int32) // top_count
    slot_table = jnp.zeros((expert_count * row_cap,), jnp.int32).at[slot_ids].set(token_ids + 1)
    own_columns = lax.dynamic_slice_in_dim(normed, lax.axis_index("tp") * half_width, half_width, 1)
    sendbuf = fill_rows(own_columns, slot_table).reshape(
        ep_count, local_experts, row_cap, half_width
    )
    arrived = lax.all_to_all(sendbuf, "ep", split_axis=0, concat_axis=0, tiled=True)
    arrived = lax.all_gather(arrived, "tp", axis=3, tiled=True)
    gate_act = jnp.einsum("secd,edf->secf", arrived, w_gate, preferred_element_type=jnp.float32)
    up_act = jnp.einsum("secd,edf->secf", arrived, w_up, preferred_element_type=jnp.float32)
    hidden = (jax.nn.silu(gate_act) * up_act).astype(jnp.bfloat16)
    partial_out = jnp.einsum("secf,efd->secd", hidden, w_down, preferred_element_type=jnp.float32)
    results = lax.psum_scatter(
        partial_out.astype(jnp.bfloat16), "tp", scatter_dimension=3, tiled=True
    )
    returned = lax.all_to_all(results, "ep", split_axis=0, concat_axis=0, tiled=True).reshape(
        expert_count * row_cap, half_width
    )
    picked = returned[slot_ids].astype(jnp.float32).reshape(tok_dev, top_count, half_width)
    mixed_rows = jnp.sum(picked * gate_prob[:, :, None], axis=1)
    squares = jnp.sum(mixed_rows * mixed_rows, axis=1)
    total_squares = lax.psum(squares, "tp")
    inv_rms = lax.rsqrt(total_squares / model_width + EPS)
    return (mixed_rows * inv_rms[:, None] * out_gain).astype(jnp.bfloat16)


def dot(a, b):
    return jnp.dot(a, b, preferred_element_type=jnp.float32)


def iota(shape, dim):
    return lax.broadcasted_iota(jnp.int32, shape, dim)


def pack_kernel(members, width, cap, *refs):
    sources, refs = refs[:4], refs[4:]
    outs, map_ref, refs = refs[:GROUPS], refs[GROUPS], refs[GROUPS + 1 :]
    copies = [
        pltpu.make_async_copy(source, target, refs[4].at[i])
        for i, (source, target) in enumerate(zip(sources, refs[:4]))
    ]
    for copy in copies:
        copy.start()
    tok_ref, gain_ref, route_ref, prob_ref = refs[:4]
    half = cap // 2
    my_group = lax.axis_index("ep") // members
    my_half = lax.axis_index("tp")
    tok_dev, model_width = tok_ref.shape
    copies[2].wait()
    copies[3].wait()
    routes = route_ref[...]
    probs = prob_ref[...]
    first = routes[0:1]
    group = jnp.zeros_like(first)
    for g in range(1, GROUPS):
        group += (first >= g * width).astype(jnp.int32)
    member = (group == iota((8, tok_dev), 0)).astype(jnp.float32)
    before = (iota((tok_dev, tok_dev), 0) < iota((tok_dev, tok_dev), 1)).astype(jnp.bfloat16)
    earlier = dot(member.astype(jnp.bfloat16), before)
    rank = jnp.sum(earlier * member, axis=0, keepdims=True).astype(jnp.int32)
    relative = group ^ my_group
    send_slot = iota((GROUPS * half, tok_dev), 0)
    pick = (
        (relative == send_slot // half) & (rank == send_slot % half + my_half * half)
    ).astype(jnp.bfloat16)
    lane = iota((LANES, tok_dev), 0)
    weight = jnp.zeros((LANES, tok_dev), jnp.float32)
    for k in range(routes.shape[0]):
        weight += jnp.where(
            routes[k : k + 1] - group * width == lane % width, probs[k : k + 1], 0.0
        )
    high = weight.astype(jnp.bfloat16).astype(jnp.float32)
    rest = weight - high
    middle = rest.astype(jnp.bfloat16).astype(jnp.float32)
    low = rest - middle
    terms = jnp.where(
        lane < width,
        high,
        jnp.where(lane < 2 * width, middle, jnp.where(lane < TERMS * width, low, 0.0)),
    ).astype(jnp.bfloat16)
    extra = lax.dot_general(
        pick, terms, (((1,), (1,)), ((), ())), preferred_element_type=jnp.float32
    ).astype(jnp.bfloat16)
    map_ref[...] = (relative * cap + rank == iota((GROUPS * cap, tok_dev), 0)).astype(jnp.bfloat16)
    copies[0].wait()
    copies[1].wait()
    floats = tok_ref[...].astype(jnp.float32)
    inv = lax.rsqrt(jnp.sum(floats * floats, axis=-1, keepdims=True) / model_width + EPS)
    normed = (floats * inv * gain_ref[...]).astype(jnp.bfloat16)
    rows = dot(pick, normed).astype(jnp.bfloat16)
    for k in range(GROUPS):
        outs[k][:, :model_width] = rows[k * half : (k + 1) * half]
        outs[k][:, model_width:] = extra[k * half : (k + 1) * half]


def load_kernel(wg_ref, wu_ref, wd_ref, map_ref, wg_out, wu_out, wd_out, map_out, sems):
    copies = [
        pltpu.make_async_copy(source.at[e], target.at[e], sems.at[i, e])
        for i, (source, target) in enumerate(
            ((wg_ref, wg_out), (wu_ref, wu_out), (wd_ref, wd_out))
        )
        for e in range(wg_ref.shape[0])
    ]
    for copy in copies:
        copy.start()
    map_out[...] = map_ref[...].astype(jnp.float32).T.astype(jnp.bfloat16)
    for copy in copies:
        copy.wait()


def expert_kernel(chunks, members, width, *refs):
    pieces, refs = refs[: 2 * chunks], refs[2 * chunks :]
    weights, outs, rows_ref = refs[:6], refs[6:-1], refs[-1]
    me = lax.axis_index("ep") % members
    local_experts, model_width, _ = weights[0].shape
    half = pieces[0].shape[0]
    for i, piece in enumerate(pieces):
        rows_ref[i * half : (i + 1) * half, :] = piece[...]
    used = len(pieces) * half
    if used < rows_ref.shape[0]:
        rows_ref[used:, :] = jnp.zeros((rows_ref.shape[0] - used, rows_ref.shape[1]), rows_ref.dtype)
    rows = rows_ref[:, :model_width]
    terms = rows_ref[:, model_width:].astype(jnp.float32)
    lane = iota(terms.shape, 1)
    hidden = []
    for e in range(local_experts):
        wanted = (lane % width == me * local_experts + e) & (lane < TERMS * width)
        weight = jnp.sum(jnp.where(wanted, terms, 0.0), axis=1, keepdims=True)
        for wg_ref, wu_ref in (weights[:2], weights[3:5]):
            gate_act = dot(rows, wg_ref[e])
            up_act = dot(rows, wu_ref[e])
            act = gate_act / (1.0 + jnp.exp(-gate_act)) * up_act
            hidden.append((act * weight).astype(jnp.bfloat16))
    hidden = jnp.concatenate(hidden, axis=1)
    down = [ref[e] for e in range(local_experts) for ref in (weights[2], weights[5])]
    total = dot(hidden, jnp.concatenate(down, axis=0))
    for c in range(chunks):
        outs[2 * c][...] = total[2 * c * half : (2 * c + 1) * half]
        outs[2 * c + 1][...] = total[(2 * c + 1) * half : (2 * c + 2) * half].astype(jnp.bfloat16)


def join_kernel(keep_ref, recv_ref, same_ref, other_ref, rows_ref):
    rows = keep_ref[...] + recv_ref[...].astype(jnp.float32)
    model_width = rows.shape[1]
    mean = jnp.sum(rows * rows, axis=1, keepdims=True) / model_width
    rows_ref[...] = (rows * lax.rsqrt(mean + EPS)).astype(jnp.bfloat16)
    half_width = same_ref.shape[1]
    my_half = lax.axis_index("tp")
    same_ref[...] = rows_ref[:, pl.ds(pl.multiple_of(my_half * half_width, half_width), half_width)]
    other_ref[...] = rows_ref[
        :, pl.ds(pl.multiple_of((1 - my_half) * half_width, half_width), half_width)
    ]


def close_kernel(cap, map_ref, gain_ref, *refs):
    parts, out_ref, rows_ref = refs[: 2 * GROUPS], refs[-2], refs[-1]
    half = cap // 2
    my_half = lax.axis_index("tp")
    for k in range(GROUPS):
        same = pl.multiple_of(k * cap + my_half * half, half)
        other = pl.multiple_of(k * cap + (1 - my_half) * half, half)
        rows_ref[pl.ds(same, half), :] = parts[2 * k][...]
        rows_ref[pl.ds(other, half), :] = parts[2 * k + 1][...]
    out_ref[...] = (dot(map_ref[...], rows_ref[...]) * gain_ref[...]).astype(jnp.bfloat16)


def call(kernel, outs, args, limit, scratch=(), in_specs=None):
    return pl.pallas_call(
        kernel,
        out_shape=outs,
        in_specs=in_specs or [pl.BlockSpec(memory_space=pltpu.VMEM)] * len(args),
        scratch_shapes=scratch,
        compiler_params=pltpu.CompilerParams(vmem_limit_bytes=limit * MIB),
    )(*args)


STAGES = ((0, 1), (3,), (2,))


def dense_body(tokens, in_gain, routing, gate_prob, w_gate, w_up, w_down, out_gain):
    ep_count = lax.axis_size("ep")
    local_experts, model_width, _ = w_gate.shape
    tok_dev, top_count = routing.shape
    half_width = out_gain.shape[0]
    width = local_experts * ep_count // GROUPS
    members = width // local_experts
    cap = tok_dev * top_count // (2 * width)
    half = cap // 2
    sds = jax.ShapeDtypeStruct
    bf16, f32 = jnp.bfloat16, jnp.float32
    block = sds((half, model_width + LANES), bf16)
    anywhere = pl.BlockSpec(memory_space=pltpu.HBM)
    in_vmem = pl.BlockSpec(memory_space=pltpu.VMEM)

    def far_ep(i, k):
        return ((i // members) ^ k) * members + i % members

    def hop(value, k):
        return lax.ppermute(value, "ep", [(i, far_ep(i, k)) for i in range(ep_count)])

    def hop_swap(value, k):
        pairs = [
            (2 * i + t, 2 * far_ep(i, k) + 1 - t) for i in range(ep_count) for t in range(2)
        ]
        return lax.ppermute(value, ("ep", "tp"), pairs)

    def cross(value):
        return lax.ppermute(value, "ep", [(i, i ^ 1) for i in range(ep_count)])

    def swap(value):
        return lax.ppermute(value, "tp", [(0, 1), (1, 0)])

    def held(value):
        return pltpu.with_memory_space_constraint(value, pltpu.HBM)

    routes_t, probs_t = held(routing.T), held(gate_prob.T)
    tokens, gain_row = held(tokens), held(in_gain.reshape(1, -1))
    w_gate, w_up, w_down = held(w_gate), held(w_up), held(w_down)
    *packed, slot_map = call(
        functools.partial(pack_kernel, members, width, cap),
        [block] * GROUPS + [sds((GROUPS * cap, tok_dev), bf16)],
        (tokens, gain_row, routes_t, probs_t),
        12,
        (
            pltpu.VMEM(tokens.shape, bf16),
            pltpu.VMEM((1, model_width), f32),
            pltpu.VMEM(routes_t.shape, jnp.int32),
            pltpu.VMEM(probs_t.shape, f32),
            pltpu.SemaphoreType.DMA((4,)),
        ),
        [anywhere] * 4,
    )
    *weights, token_map = call(
        load_kernel,
        [sds(w.shape, bf16) for w in (w_gate, w_up, w_down)]
        + [sds((tok_dev, GROUPS * cap), bf16)],
        (w_gate, w_up, w_down, slot_map),
        12,
        (pltpu.SemaphoreType.DMA((3, local_experts)),),
        [anywhere] * 3 + [in_vmem],
    )
    arrived = [packed[0]] + [hop(packed[k], k) for k in range(1, GROUPS)]
    weights += [swap(w) for w in (w_gate, w_up, w_down)]
    weights = [pltpu.with_memory_space_constraint(w, pltpu.VMEM) for w in weights]

    back = [None] * (2 * GROUPS)

    def experts(ks):
        pieces = []
        for k in ks:
            pieces += [arrived[k], cross(arrived[k])]
        n = len(ks)
        sums = call(
            functools.partial(expert_kernel, n, members, width),
            [sds((half, model_width), f32), sds((half, model_width), bf16)] * n,
            (*pieces, *weights),
            20,
            (pltpu.VMEM((max(n * cap, LANES), model_width + LANES), bf16),),
        )
        for c, k in enumerate(ks):
            same, other = call(
                join_kernel,
                [sds((half, half_width), bf16)] * 2,
                (sums[2 * c], cross(sums[2 * c + 1])),
                8,
                (pltpu.VMEM((half, model_width), bf16),),
            )
            if k == 0:
                back[:2] = same, swap(other)
            else:
                back[2 * k] = hop(same, k)
                back[2 * k + 1] = hop_swap(other, k)

    for ks in STAGES:
        experts(ks)
    return call(
        functools.partial(close_kernel, cap),
        sds((tok_dev, half_width), bf16),
        (token_map, out_gain.reshape(1, -1), *back),
        8,
        (pltpu.VMEM((GROUPS * cap, half_width), bf16),),
    )


def solution(mesh):
    placed = (
        P(("grp", "ep"), None),
        P(),
        P(("grp", "ep"), None),
        P(("grp", "ep"), None),
        P("ep", None, "tp"),
        P("ep", None, "tp"),
        P("ep", "tp", None),
        P("tp"),
    )

    def step(*args):
        routing, w_gate = args[2], args[4]
        width = w_gate.shape[0] // GROUPS
        members = mesh.shape["ep"] // GROUPS
        dense = routing.shape[1] == width and members == 2 and mesh.shape["tp"] == 2

        def body(*shards):
            return (dense_body if dense else sparse_body)(*shards)

        whole = jax.shard_map(
            body, mesh=mesh, in_specs=placed, out_specs=P(("grp", "ep"), "tp"), check_vma=False
        )
        return whole(*args)

    return step
```

```python
import functools

import jax
import jax.numpy as jnp
from jax import lax
from jax.experimental import pallas as pl
from jax.experimental.pallas import tpu as pltpu
from jax.sharding import PartitionSpec as P

GROUPS = 4


EPS = 1e-06
LANES = 128
TERMS = 3
MIB = 1 << 20


def slot_ranks(flat_routes, expert_count):
    matches = (flat_routes[:, None] == jnp.arange(expert_count, dtype=jnp.int32)[None, :]).astype(
        jnp.int32
    )
    earlier = jnp.cumsum(matches, axis=0) - matches
    return jnp.sum(earlier * matches, axis=1)


def fill_rows(source, entries):
    filled = entries > 0
    return jnp.where(
        filled[:, None], source[jnp.maximum(entries - 1, 0)], jnp.zeros((), source.dtype)
    )


def sparse_body(tokens, in_gain, routing, gate_prob, w_gate, w_up, w_down, out_gain):
    ep_count = lax.axis_size("ep")
    local_experts = w_gate.shape[0]
    expert_count = local_experts * ep_count
    tok_dev, top_count = routing.shape
    model_width = tokens.shape[1]
    half_width = out_gain.shape[0]
    group_width = expert_count // GROUPS
    row_cap = max(2, tok_dev * top_count // (2 * group_width))
    floats = tokens.astype(jnp.float32)
    normed = (
        floats * lax.rsqrt(jnp.mean(floats * floats, axis=-1, keepdims=True) + EPS) * in_gain
    ).astype(jnp.bfloat16)
    flat_routes = routing.reshape(-1)
    slot_rank = slot_ranks(flat_routes, expert_count)
    slot_ids = flat_routes * row_cap + slot_rank
    token_ids = jnp.arange(tok_dev * top_count, dtype=jnp.int32) // top_count
    slot_table = jnp.zeros((expert_count * row_cap,), jnp.int32).at[slot_ids].set(token_ids + 1)
    own_columns = lax.dynamic_slice_in_dim(normed, lax.axis_index("tp") * half_width, half_width, 1)
    sendbuf = fill_rows(own_columns, slot_table).reshape(
        ep_count, local_experts, row_cap, half_width
    )
    arrived = lax.all_to_all(sendbuf, "ep", split_axis=0, concat_axis=0, tiled=True)
    arrived = lax.all_gather(arrived, "tp", axis=3, tiled=True)
    gate_act = jnp.einsum("secd,edf->secf", arrived, w_gate, preferred_element_type=jnp.float32)
    up_act = jnp.einsum("secd,edf->secf", arrived, w_up, preferred_element_type=jnp.float32)
    hidden = (jax.nn.silu(gate_act) * up_act).astype(jnp.bfloat16)
    partial_out = jnp.einsum("secf,efd->secd", hidden, w_down, preferred_element_type=jnp.float32)
    results = lax.psum_scatter(
        partial_out.astype(jnp.bfloat16), "tp", scatter_dimension=3, tiled=True
    )
    returned = lax.all_to_all(results, "ep", split_axis=0, concat_axis=0, tiled=True).reshape(
        expert_count * row_cap, half_width
    )
    picked = returned[slot_ids].astype(jnp.float32).reshape(tok_dev, top_count, half_width)
    mixed_rows = jnp.sum(picked * gate_prob[:, :, None], axis=1)
    squares = jnp.sum(mixed_rows * mixed_rows, axis=1)
    total_squares = lax.psum(squares, "tp")
    inv_rms = lax.rsqrt(total_squares / model_width + EPS)
    return (mixed_rows * inv_rms[:, None] * out_gain).astype(jnp.bfloat16)


def dot(a, b):
    return jnp.dot(a, b, preferred_element_type=jnp.float32)


def iota(shape, dim):
    return lax.broadcasted_iota(jnp.int32, shape, dim)


def pack_kernel(members, width, cap, *refs):
    sources, refs = refs[:4], refs[4:]
    outs, map_ref, refs = refs[:GROUPS], refs[GROUPS], refs[GROUPS + 1 :]
    copies = [
        pltpu.make_async_copy(source, target, refs[4].at[i])
        for i, (source, target) in enumerate(zip(sources, refs[:4]))
    ]
    for copy in copies:
        copy.start()
    tok_ref, gain_ref, route_ref, prob_ref = refs[:4]
    half = cap // 2
    my_group = lax.axis_index("ep") // members
    my_half = lax.axis_index("tp")
    tok_dev, model_width = tok_ref.shape
    copies[2].wait()
    copies[3].wait()
    routes = route_ref[...]
    probs = prob_ref[...]
    first = routes[0:1]
    group = jnp.zeros_like(first)
    for g in range(1, GROUPS):
        group += (first >= g * width).astype(jnp.int32)
    member = (group == iota((8, tok_dev), 0)).astype(jnp.float32)
    before = (iota((tok_dev, tok_dev), 0) < iota((tok_dev, tok_dev), 1)).astype(jnp.bfloat16)
    earlier = dot(member.astype(jnp.bfloat16), before)
    rank = jnp.sum(earlier * member, axis=0, keepdims=True).astype(jnp.int32)
    relative = group - my_group
    relative += jnp.where(relative < 0, GROUPS, 0)
    send_slot = iota((GROUPS * half, tok_dev), 0)
    pick = (
        (relative == send_slot // half) & (rank == send_slot % half + my_half * half)
    ).astype(jnp.bfloat16)
    lane = iota((LANES, tok_dev), 0)
    weight = jnp.zeros((LANES, tok_dev), jnp.float32)
    for k in range(routes.shape[0]):
        weight += jnp.where(
            routes[k : k + 1] - group * width == lane % width, probs[k : k + 1], 0.0
        )
    high = weight.astype(jnp.bfloat16).astype(jnp.float32)
    rest = weight - high
    middle = rest.astype(jnp.bfloat16).astype(jnp.float32)
    low = rest - middle
    terms = jnp.where(
        lane < width,
        high,
        jnp.where(lane < 2 * width, middle, jnp.where(lane < TERMS * width, low, 0.0)),
    ).astype(jnp.bfloat16)
    extra = lax.dot_general(
        pick, terms, (((1,), (1,)), ((), ())), preferred_element_type=jnp.float32
    ).astype(jnp.bfloat16)
    map_ref[...] = (relative * cap + rank == iota((GROUPS * cap, tok_dev), 0)).astype(jnp.bfloat16)
    copies[0].wait()
    copies[1].wait()
    floats = tok_ref[...].astype(jnp.float32)
    inv = lax.rsqrt(jnp.sum(floats * floats, axis=-1, keepdims=True) / model_width + EPS)
    normed = (floats * inv * gain_ref[...]).astype(jnp.bfloat16)
    rows = dot(pick, normed).astype(jnp.bfloat16)
    for k in range(GROUPS):
        outs[k][:, :model_width] = rows[k * half : (k + 1) * half]
        outs[k][:, model_width:] = extra[k * half : (k + 1) * half]


def load_kernel(wg_ref, wu_ref, wd_ref, map_ref, wg_out, wu_out, wd_out, map_out, sems):
    copies = [
        pltpu.make_async_copy(source.at[e], target.at[e], sems.at[i, e])
        for i, (source, target) in enumerate(
            ((wg_ref, wg_out), (wu_ref, wu_out), (wd_ref, wd_out))
        )
        for e in range(wg_ref.shape[0])
    ]
    for copy in copies:
        copy.start()
    map_out[...] = map_ref[...].astype(jnp.float32).T.astype(jnp.bfloat16)
    for copy in copies:
        copy.wait()


def expert_kernel(chunks, members, width, *refs):
    pieces, refs = refs[: 2 * chunks], refs[2 * chunks :]
    weights, outs, rows_ref = refs[:6], refs[6:-1], refs[-1]
    me = lax.axis_index("ep") % members
    local_experts, model_width, _ = weights[0].shape
    half = pieces[0].shape[0]
    for i, piece in enumerate(pieces):
        rows_ref[i * half : (i + 1) * half, :] = piece[...]
    used = len(pieces) * half
    if used < rows_ref.shape[0]:
        rows_ref[used:, :] = jnp.zeros((rows_ref.shape[0] - used, rows_ref.shape[1]), rows_ref.dtype)
    rows = rows_ref[:, :model_width]
    terms = rows_ref[:, model_width:].astype(jnp.float32)
    lane = iota(terms.shape, 1)
    hidden = []
    for e in range(local_experts):
        wanted = (lane % width == me * local_experts + e) & (lane < TERMS * width)
        weight = jnp.sum(jnp.where(wanted, terms, 0.0), axis=1, keepdims=True)
        for wg_ref, wu_ref in (weights[:2], weights[3:5]):
            gate_act = dot(rows, wg_ref[e])
            up_act = dot(rows, wu_ref[e])
            act = gate_act / (1.0 + jnp.exp(-gate_act)) * up_act
            hidden.append((act * weight).astype(jnp.bfloat16))
    hidden = jnp.concatenate(hidden, axis=1)
    down = [ref[e] for e in range(local_experts) for ref in (weights[2], weights[5])]
    total = dot(hidden, jnp.concatenate(down, axis=0))
    for c in range(chunks):
        outs[2 * c][...] = total[2 * c * half : (2 * c + 1) * half]
        outs[2 * c + 1][...] = total[(2 * c + 1) * half : (2 * c + 2) * half].astype(jnp.bfloat16)


def join_kernel(keep_ref, recv_ref, same_ref, other_ref, rows_ref):
    rows = keep_ref[...] + recv_ref[...].astype(jnp.float32)
    model_width = rows.shape[1]
    mean = jnp.sum(rows * rows, axis=1, keepdims=True) / model_width
    rows_ref[...] = (rows * lax.rsqrt(mean + EPS)).astype(jnp.bfloat16)
    half_width = same_ref.shape[1]
    my_half = lax.axis_index("tp")
    same_ref[...] = rows_ref[:, pl.ds(pl.multiple_of(my_half * half_width, half_width), half_width)]
    other_ref[...] = rows_ref[
        :, pl.ds(pl.multiple_of((1 - my_half) * half_width, half_width), half_width)
    ]


def join_whole_kernel(keep_ref, recv_ref, out_ref):
    rows = keep_ref[...] + recv_ref[...].astype(jnp.float32)
    mean = jnp.sum(rows * rows, axis=1, keepdims=True) / rows.shape[1]
    out_ref[...] = (rows * lax.rsqrt(mean + EPS)).astype(jnp.bfloat16)


def close_kernel(cap, map_ref, gain_ref, *refs):
    parts, out_ref, rows_ref = refs[: 2 * GROUPS], refs[-2], refs[-1]
    half = cap // 2
    half_width = out_ref.shape[1]
    my_half = lax.axis_index("tp")

    def features(ref):
        if ref.shape[1] == half_width:
            return ref[...]
        return ref[:, pl.ds(pl.multiple_of(my_half * half_width, half_width), half_width)]

    for k in range(GROUPS):
        same = pl.multiple_of(k * cap + my_half * half, half)
        other = pl.multiple_of(k * cap + (1 - my_half) * half, half)
        rows_ref[pl.ds(same, half), :] = features(parts[2 * k])
        rows_ref[pl.ds(other, half), :] = features(parts[2 * k + 1])
    out_ref[...] = (dot(map_ref[...], rows_ref[...]) * gain_ref[...]).astype(jnp.bfloat16)


def call(kernel, outs, args, limit, scratch=(), in_specs=None):
    return pl.pallas_call(
        kernel,
        out_shape=outs,
        in_specs=in_specs or [pl.BlockSpec(memory_space=pltpu.VMEM)] * len(args),
        scratch_shapes=scratch,
        compiler_params=pltpu.CompilerParams(vmem_limit_bytes=limit * MIB),
    )(*args)


STAGES = ((0, 1), (2,), (3,))
SPLIT = (3,)


def dense_body(tokens, in_gain, routing, gate_prob, w_gate, w_up, w_down, out_gain):
    ep_count = lax.axis_size("ep")
    local_experts, model_width, _ = w_gate.shape
    tok_dev, top_count = routing.shape
    half_width = out_gain.shape[0]
    width = local_experts * ep_count // GROUPS
    members = width // local_experts
    cap = tok_dev * top_count // (2 * width)
    half = cap // 2
    sds = jax.ShapeDtypeStruct
    bf16, f32 = jnp.bfloat16, jnp.float32
    block = sds((half, model_width + LANES), bf16)
    anywhere = pl.BlockSpec(memory_space=pltpu.HBM)
    in_vmem = pl.BlockSpec(memory_space=pltpu.VMEM)

    def far_ep(i, k):
        return (i // members + k) % GROUPS * members + i % members

    def hop(value, k):
        return lax.ppermute(value, "ep", [(i, far_ep(i, k)) for i in range(ep_count)])

    def hop_swap(value, k):
        pairs = [
            (2 * i + t, 2 * far_ep(i, k) + 1 - t) for i in range(ep_count) for t in range(2)
        ]
        return lax.ppermute(value, ("ep", "tp"), pairs)

    def cross(value):
        return lax.ppermute(value, "ep", [(i, i ^ 1) for i in range(ep_count)])

    def swap(value):
        return lax.ppermute(value, "tp", [(0, 1), (1, 0)])

    def held(value):
        return pltpu.with_memory_space_constraint(value, pltpu.HBM)

    routes_t, probs_t = held(routing.T), held(gate_prob.T)
    tokens, gain_row = held(tokens), held(in_gain.reshape(1, -1))
    w_gate, w_up, w_down = held(w_gate), held(w_up), held(w_down)
    *packed, slot_map = call(
        functools.partial(pack_kernel, members, width, cap),
        [block] * GROUPS + [sds((GROUPS * cap, tok_dev), bf16)],
        (tokens, gain_row, routes_t, probs_t),
        12,
        (
            pltpu.VMEM(tokens.shape, bf16),
            pltpu.VMEM((1, model_width), f32),
            pltpu.VMEM(routes_t.shape, jnp.int32),
            pltpu.VMEM(probs_t.shape, f32),
            pltpu.SemaphoreType.DMA((4,)),
        ),
        [anywhere] * 4,
    )
    *weights, token_map = call(
        load_kernel,
        [sds(w.shape, bf16) for w in (w_gate, w_up, w_down)]
        + [sds((tok_dev, GROUPS * cap), bf16)],
        (w_gate, w_up, w_down, slot_map),
        12,
        (pltpu.SemaphoreType.DMA((3, local_experts)),),
        [anywhere] * 3 + [in_vmem],
    )
    arrived = [packed[0]] + [hop(packed[k], k) for k in range(1, GROUPS)]
    weights += [swap(w) for w in (w_gate, w_up, w_down)]
    weights = [pltpu.with_memory_space_constraint(w, pltpu.VMEM) for w in weights]

    back = [None] * (2 * GROUPS)

    def experts(ks):
        pieces = []
        for k in ks:
            pieces += [arrived[k], cross(arrived[k])]
        n = len(ks)
        sums = call(
            functools.partial(expert_kernel, n, members, width),
            [sds((half, model_width), f32), sds((half, model_width), bf16)] * n,
            (*pieces, *weights),
            20,
            (pltpu.VMEM((max(n * cap, LANES), model_width + LANES), bf16),),
        )
        for c, k in enumerate(ks):
            keep, recv = sums[2 * c], cross(sums[2 * c + 1])
            if k in SPLIT:
                same, other = call(
                    join_kernel,
                    [sds((half, half_width), bf16)] * 2,
                    (keep, recv),
                    8,
                    (pltpu.VMEM((half, model_width), bf16),),
                )
                back[2 * k] = hop(same, -k)
                back[2 * k + 1] = hop_swap(other, -k)
            else:
                mixed = call(join_whole_kernel, sds((half, model_width), bf16), (keep, recv), 8)
                home = hop(mixed, -k) if k else mixed
                back[2 * k : 2 * k + 2] = home, swap(home)

    for ks in STAGES:
        experts(ks)
    return call(
        functools.partial(close_kernel, cap),
        sds((tok_dev, half_width), bf16),
        (token_map, out_gain.reshape(1, -1), *back),
        8,
        (pltpu.VMEM((GROUPS * cap, half_width), bf16),),
    )


def solution(mesh):
    placed = (
        P(("grp", "ep"), None),
        P(),
        P(("grp", "ep"), None),
        P(("grp", "ep"), None),
        P("ep", None, "tp"),
        P("ep", None, "tp"),
        P("ep", "tp", None),
        P("tp"),
    )

    def step(*args):
        routing, w_gate = args[2], args[4]
        width = w_gate.shape[0] // GROUPS
        members = mesh.shape["ep"] // GROUPS
        dense = routing.shape[1] == width and members == 2 and mesh.shape["tp"] == 2

        def body(*shards):
            return (dense_body if dense else sparse_body)(*shards)

        whole = jax.shard_map(
            body, mesh=mesh, in_specs=placed, out_specs=P(("grp", "ep"), "tp"), check_vma=False
        )
        return whole(*args)

    return step
```

```python
import functools

import jax
import jax.numpy as jnp
from jax import lax
from jax.experimental import pallas as pl
from jax.experimental.pallas import tpu as pltpu
from jax.sharding import PartitionSpec as P

GROUPS = 4


EPS = 1e-06
LANES = 128
TERMS = 3
MIB = 1 << 20


def slot_ranks(flat_routes, expert_count):
    matches = (flat_routes[:, None] == jnp.arange(expert_count, dtype=jnp.int32)[None, :]).astype(
        jnp.int32
    )
    earlier = jnp.cumsum(matches, axis=0) - matches
    return jnp.sum(earlier * matches, axis=1)


def fill_rows(source, entries):
    filled = entries > 0
    return jnp.where(
        filled[:, None], source[jnp.maximum(entries - 1, 0)], jnp.zeros((), source.dtype)
    )


def sparse_body(tokens, in_gain, routing, gate_prob, w_gate, w_up, w_down, out_gain):
    ep_count = lax.axis_size("ep")
    local_experts = w_gate.shape[0]
    expert_count = local_experts * ep_count
    tok_dev, top_count = routing.shape
    model_width = tokens.shape[1]
    half_width = out_gain.shape[0]
    group_width = expert_count // GROUPS
    row_cap = max(2, tok_dev * top_count // (2 * group_width))
    floats = tokens.astype(jnp.float32)
    normed = (
        floats * lax.rsqrt(jnp.mean(floats * floats, axis=-1, keepdims=True) + EPS) * in_gain
    ).astype(jnp.bfloat16)
    flat_routes = routing.reshape(-1)
    slot_rank = slot_ranks(flat_routes, expert_count)
    slot_ids = flat_routes * row_cap + slot_rank
    token_ids = jnp.arange(tok_dev * top_count, dtype=jnp.int32) // top_count
    slot_table = jnp.zeros((expert_count * row_cap,), jnp.int32).at[slot_ids].set(token_ids + 1)
    own_columns = lax.dynamic_slice_in_dim(normed, lax.axis_index("tp") * half_width, half_width, 1)
    sendbuf = fill_rows(own_columns, slot_table).reshape(
        ep_count, local_experts, row_cap, half_width
    )
    arrived = lax.all_to_all(sendbuf, "ep", split_axis=0, concat_axis=0, tiled=True)
    arrived = lax.all_gather(arrived, "tp", axis=3, tiled=True)
    gate_act = jnp.einsum("secd,edf->secf", arrived, w_gate, preferred_element_type=jnp.float32)
    up_act = jnp.einsum("secd,edf->secf", arrived, w_up, preferred_element_type=jnp.float32)
    hidden = (jax.nn.silu(gate_act) * up_act).astype(jnp.bfloat16)
    partial_out = jnp.einsum("secf,efd->secd", hidden, w_down, preferred_element_type=jnp.float32)
    results = lax.psum_scatter(
        partial_out.astype(jnp.bfloat16), "tp", scatter_dimension=3, tiled=True
    )
    returned = lax.all_to_all(results, "ep", split_axis=0, concat_axis=0, tiled=True).reshape(
        expert_count * row_cap, half_width
    )
    picked = returned[slot_ids].astype(jnp.float32).reshape(tok_dev, top_count, half_width)
    mixed_rows = jnp.sum(picked * gate_prob[:, :, None], axis=1)
    squares = jnp.sum(mixed_rows * mixed_rows, axis=1)
    total_squares = lax.psum(squares, "tp")
    inv_rms = lax.rsqrt(total_squares / model_width + EPS)
    return (mixed_rows * inv_rms[:, None] * out_gain).astype(jnp.bfloat16)


def dot(a, b):
    return jnp.dot(a, b, preferred_element_type=jnp.float32)


def iota(shape, dim):
    return lax.broadcasted_iota(jnp.int32, shape, dim)


def pack_kernel(members, width, cap, *refs):
    sources, refs = refs[:4], refs[4:]
    outs, map_ref, refs = refs[:GROUPS], refs[GROUPS], refs[GROUPS + 1 :]
    copies = [
        pltpu.make_async_copy(source, target, refs[4].at[i])
        for i, (source, target) in enumerate(zip(sources, refs[:4]))
    ]
    for copy in copies:
        copy.start()
    tok_ref, gain_ref, route_ref, prob_ref = refs[:4]
    half = cap // 2
    my_group = lax.axis_index("ep") // members
    my_half = lax.axis_index("tp")
    tok_dev, model_width = tok_ref.shape
    copies[2].wait()
    copies[3].wait()
    routes = route_ref[...]
    probs = prob_ref[...]
    first = routes[0:1]
    group = jnp.zeros_like(first)
    for g in range(1, GROUPS):
        group += (first >= g * width).astype(jnp.int32)
    member = (group == iota((8, tok_dev), 0)).astype(jnp.float32)
    before = (iota((tok_dev, tok_dev), 0) < iota((tok_dev, tok_dev), 1)).astype(jnp.bfloat16)
    earlier = dot(member.astype(jnp.bfloat16), before)
    rank = jnp.sum(earlier * member, axis=0, keepdims=True).astype(jnp.int32)
    relative = group - my_group
    relative += jnp.where(relative < 0, GROUPS, 0)
    send_slot = iota((GROUPS * half, tok_dev), 0)
    pick = (
        (relative == send_slot // half) & (rank == send_slot % half + my_half * half)
    ).astype(jnp.bfloat16)
    lane = iota((LANES, tok_dev), 0)
    weight = jnp.zeros((LANES, tok_dev), jnp.float32)
    for k in range(routes.shape[0]):
        weight += jnp.where(
            routes[k : k + 1] - group * width == lane % width, probs[k : k + 1], 0.0
        )
    high = weight.astype(jnp.bfloat16).astype(jnp.float32)
    rest = weight - high
    middle = rest.astype(jnp.bfloat16).astype(jnp.float32)
    low = rest - middle
    terms = jnp.where(
        lane < width,
        high,
        jnp.where(lane < 2 * width, middle, jnp.where(lane < TERMS * width, low, 0.0)),
    ).astype(jnp.bfloat16)
    extra = lax.dot_general(
        pick, terms, (((1,), (1,)), ((), ())), preferred_element_type=jnp.float32
    ).astype(jnp.bfloat16)
    map_ref[...] = (relative * cap + rank == iota((GROUPS * cap, tok_dev), 0)).astype(jnp.bfloat16)
    copies[0].wait()
    copies[1].wait()
    floats = tok_ref[...].astype(jnp.float32)
    inv = lax.rsqrt(jnp.sum(floats * floats, axis=-1, keepdims=True) / model_width + EPS)
    normed = (floats * inv * gain_ref[...]).astype(jnp.bfloat16)
    rows = dot(pick, normed).astype(jnp.bfloat16)
    for k in range(GROUPS):
        outs[k][:, :model_width] = rows[k * half : (k + 1) * half]
        outs[k][:, model_width:] = extra[k * half : (k + 1) * half]


def load_kernel(wg_ref, wu_ref, wd_ref, map_ref, wg_out, wu_out, wd_out, map_out, sems):
    copies = [
        pltpu.make_async_copy(source.at[e], target.at[e], sems.at[i, e])
        for i, (source, target) in enumerate(
            ((wg_ref, wg_out), (wu_ref, wu_out), (wd_ref, wd_out))
        )
        for e in range(wg_ref.shape[0])
    ]
    for copy in copies:
        copy.start()
    map_out[...] = map_ref[...].astype(jnp.float32).T.astype(jnp.bfloat16)
    for copy in copies:
        copy.wait()


def expert_kernel(chunks, members, width, *refs):
    pieces, refs = refs[: 2 * chunks], refs[2 * chunks :]
    weights, outs, rows_ref = refs[:6], refs[6:-1], refs[-1]
    me = lax.axis_index("ep") % members
    local_experts, model_width, _ = weights[0].shape
    half = pieces[0].shape[0]
    for i, piece in enumerate(pieces):
        rows_ref[i * half : (i + 1) * half, :] = piece[...]
    used = len(pieces) * half
    if used < rows_ref.shape[0]:
        rows_ref[used:, :] = jnp.zeros((rows_ref.shape[0] - used, rows_ref.shape[1]), rows_ref.dtype)
    rows = rows_ref[:, :model_width]
    terms = rows_ref[:, model_width:].astype(jnp.float32)
    lane = iota(terms.shape, 1)
    hidden = []
    for e in range(local_experts):
        wanted = (lane % width == me * local_experts + e) & (lane < TERMS * width)
        weight = jnp.sum(jnp.where(wanted, terms, 0.0), axis=1, keepdims=True)
        for wg_ref, wu_ref in (weights[:2], weights[3:5]):
            gate_act = dot(rows, wg_ref[e])
            up_act = dot(rows, wu_ref[e])
            act = gate_act / (1.0 + jnp.exp(-gate_act)) * up_act
            hidden.append((act * weight).astype(jnp.bfloat16))
    down = [ref[e] for e in range(local_experts) for ref in (weights[2], weights[5])]
    total = dot(hidden[0], down[0])
    for h, w in zip(hidden[1:], down[1:]):
        total += dot(h, w)
    for c in range(chunks):
        outs[2 * c][...] = total[2 * c * half : (2 * c + 1) * half]
        outs[2 * c + 1][...] = total[(2 * c + 1) * half : (2 * c + 2) * half].astype(jnp.bfloat16)


def join_kernel(keep_ref, recv_ref, same_ref, other_ref, rows_ref):
    rows = keep_ref[...] + recv_ref[...].astype(jnp.float32)
    model_width = rows.shape[1]
    mean = jnp.sum(rows * rows, axis=1, keepdims=True) / model_width
    rows_ref[...] = (rows * lax.rsqrt(mean + EPS)).astype(jnp.bfloat16)
    half_width = same_ref.shape[1]
    my_half = lax.axis_index("tp")
    same_ref[...] = rows_ref[:, pl.ds(pl.multiple_of(my_half * half_width, half_width), half_width)]
    other_ref[...] = rows_ref[
        :, pl.ds(pl.multiple_of((1 - my_half) * half_width, half_width), half_width)
    ]


def join_whole_kernel(keep_ref, recv_ref, out_ref):
    rows = keep_ref[...] + recv_ref[...].astype(jnp.float32)
    mean = jnp.sum(rows * rows, axis=1, keepdims=True) / rows.shape[1]
    out_ref[...] = (rows * lax.rsqrt(mean + EPS)).astype(jnp.bfloat16)


def close_kernel(cap, map_ref, gain_ref, *refs):
    parts, (out_ref, rows_ref, done_ref, sems) = refs[: 2 * GROUPS], refs[2 * GROUPS :]
    half = cap // 2
    half_width = out_ref.shape[1]
    my_half = lax.axis_index("tp")

    def features(ref):
        if ref.shape[1] == half_width:
            return ref[...]
        return ref[:, pl.ds(pl.multiple_of(my_half * half_width, half_width), half_width)]

    for k in range(GROUPS):
        same = pl.multiple_of(k * cap + my_half * half, half)
        other = pl.multiple_of(k * cap + (1 - my_half) * half, half)
        rows_ref[pl.ds(same, half), :] = features(parts[2 * k])
        rows_ref[pl.ds(other, half), :] = features(parts[2 * k + 1])
    copies = []
    block = done_ref.shape[1] // 2
    for i in range(2):
        at = slice(i * block, (i + 1) * block)
        done_ref[:, at] = (dot(map_ref[...], rows_ref[:, at]) * gain_ref[:, at]).astype(
            jnp.bfloat16
        )
        copies.append(pltpu.make_async_copy(done_ref.at[:, at], out_ref.at[:, at], sems.at[i]))
        copies[-1].start()
    for copy in copies:
        copy.wait()


def call(kernel, outs, args, limit, scratch=(), in_specs=None, **specs):
    return pl.pallas_call(
        kernel,
        out_shape=outs,
        in_specs=in_specs or [pl.BlockSpec(memory_space=pltpu.VMEM)] * len(args),
        scratch_shapes=scratch,
        **specs,
        compiler_params=pltpu.CompilerParams(vmem_limit_bytes=limit * MIB),
    )(*args)


STAGES = ((1,), (2,), (0, 3))
SPLIT = (3,)


def dense_body(tokens, in_gain, routing, gate_prob, w_gate, w_up, w_down, out_gain):
    ep_count = lax.axis_size("ep")
    local_experts, model_width, _ = w_gate.shape
    tok_dev, top_count = routing.shape
    half_width = out_gain.shape[0]
    width = local_experts * ep_count // GROUPS
    members = width // local_experts
    cap = tok_dev * top_count // (2 * width)
    half = cap // 2
    sds = jax.ShapeDtypeStruct
    bf16, f32 = jnp.bfloat16, jnp.float32
    block = sds((half, model_width + LANES), bf16)
    anywhere = pl.BlockSpec(memory_space=pltpu.HBM)
    in_vmem = pl.BlockSpec(memory_space=pltpu.VMEM)

    def far_ep(i, k):
        return (i // members + k) % GROUPS * members + i % members

    def hop(value, k):
        return lax.ppermute(value, "ep", [(i, far_ep(i, k)) for i in range(ep_count)])

    def hop_swap(value, k):
        pairs = [
            (2 * i + t, 2 * far_ep(i, k) + 1 - t) for i in range(ep_count) for t in range(2)
        ]
        return lax.ppermute(value, ("ep", "tp"), pairs)

    def cross(value):
        return lax.ppermute(value, "ep", [(i, i ^ 1) for i in range(ep_count)])

    def swap(value):
        return lax.ppermute(value, "tp", [(0, 1), (1, 0)])

    def held(value):
        return pltpu.with_memory_space_constraint(value, pltpu.HBM)

    routes_t, probs_t = held(routing.T), held(gate_prob.T)
    tokens, gain_row = held(tokens), held(in_gain.reshape(1, -1))
    w_gate, w_up, w_down = held(w_gate), held(w_up), held(w_down)
    *packed, slot_map = call(
        functools.partial(pack_kernel, members, width, cap),
        [block] * GROUPS + [sds((GROUPS * cap, tok_dev), bf16)],
        (tokens, gain_row, routes_t, probs_t),
        12,
        (
            pltpu.VMEM(tokens.shape, bf16),
            pltpu.VMEM((1, model_width), f32),
            pltpu.VMEM(routes_t.shape, jnp.int32),
            pltpu.VMEM(probs_t.shape, f32),
            pltpu.SemaphoreType.DMA((4,)),
        ),
        [anywhere] * 4,
    )
    *weights, token_map = call(
        load_kernel,
        [sds(w.shape, bf16) for w in (w_gate, w_up, w_down)]
        + [sds((tok_dev, GROUPS * cap), bf16)],
        (w_gate, w_up, w_down, slot_map),
        12,
        (pltpu.SemaphoreType.DMA((3, local_experts)),),
        [anywhere] * 3 + [in_vmem],
    )
    arrived = [packed[0]] + [hop(packed[k], k) for k in range(1, GROUPS)]
    weights += [swap(w) for w in (w_gate, w_up, w_down)]
    weights = [pltpu.with_memory_space_constraint(w, pltpu.VMEM) for w in weights]

    back = [None] * (2 * GROUPS)

    def experts(ks):
        pieces = []
        for k in ks:
            pieces += [arrived[k], cross(arrived[k])]
        n = len(ks)
        sums = call(
            functools.partial(expert_kernel, n, members, width),
            [sds((half, model_width), f32), sds((half, model_width), bf16)] * n,
            (*pieces, *weights),
            20,
            (pltpu.VMEM((max(n * cap, LANES), model_width + LANES), bf16),),
        )
        for c, k in enumerate(ks):
            keep, recv = sums[2 * c], cross(sums[2 * c + 1])
            if k in SPLIT:
                same, other = call(
                    join_kernel,
                    [sds((half, half_width), bf16)] * 2,
                    (keep, recv),
                    8,
                    (pltpu.VMEM((half, model_width), bf16),),
                )
                back[2 * k] = hop(same, -k)
                back[2 * k + 1] = hop_swap(other, -k)
            else:
                mixed = call(join_whole_kernel, sds((half, model_width), bf16), (keep, recv), 8)
                home = hop(mixed, -k) if k else mixed
                back[2 * k : 2 * k + 2] = home, swap(home)

    for ks in STAGES:
        experts(ks)
    return call(
        functools.partial(close_kernel, cap),
        sds((tok_dev, half_width), bf16),
        (token_map, out_gain.reshape(1, -1), *back),
        8,
        (
            pltpu.VMEM((GROUPS * cap, half_width), bf16),
            pltpu.VMEM((tok_dev, half_width), bf16),
            pltpu.SemaphoreType.DMA((2,)),
        ),
        out_specs=anywhere,
    )


def solution(mesh):
    placed = (
        P(("grp", "ep"), None),
        P(),
        P(("grp", "ep"), None),
        P(("grp", "ep"), None),
        P("ep", None, "tp"),
        P("ep", None, "tp"),
        P("ep", "tp", None),
        P("tp"),
    )

    def step(*args):
        routing, w_gate = args[2], args[4]
        width = w_gate.shape[0] // GROUPS
        members = mesh.shape["ep"] // GROUPS
        dense = routing.shape[1] == width and members == 2 and mesh.shape["tp"] == 2

        def body(*shards):
            return (dense_body if dense else sparse_body)(*shards)

        whole = jax.shard_map(
            body, mesh=mesh, in_specs=placed, out_specs=P(("grp", "ep"), "tp"), check_vma=False
        )
        return whole(*args)

    return step
```
